32 devices in a mesh: sp: 8 (over z, x), tp: 4 (over y, core).
Axes of the slice: x: 2, y: 2, z: 4, core: 2. Of those that a mesh axis runs over, the one named last changes fastest.
Arguments:
- inputs: bfloat16 [4, 1024, 1024], P(None, 'sp'), may hold values from -6 to 6
- norm_gain: float32 [1024], replicated, may hold values from 0.1 to 1.9
- query_weight: bfloat16 [1024, 3, 8, 64], P('sp', None, 'tp'), may hold values from -0.1875 to 0.1875
- key_weight: bfloat16 [1024, 3, 8, 64], P('sp', None, 'tp'), may hold values from -0.1875 to 0.1875
- value_weight: bfloat16 [1024, 3, 8, 64], P('sp', None, 'tp'), may hold values from -0.1875 to 0.1875
- query_gain: float32 [3, 64], replicated, may hold values from 0.1 to 1.9
- key_gain: float32 [3, 64], replicated, may hold values from 0.1 to 1.9
- out_weight: bfloat16 [8, 64, 1024], P('tp', None, 'sp'), may hold values from -0.75 to 0.75
Outputs:
- mixed: bfloat16 [4, 1024, 1024], P(None, 'sp', 'tp')
The draws below stay inside these ranges and needn't reach their ends.
All inputs are finite; a program needn't handle non-finite values.
Results may differ from the reference program's by a relative error of at most 0.02.
Values may be sent and summed in bfloat16 or wider, within the bound.
A program may use at most 64 MiB of HBM per device.

```python
import math
import jax
import jax.numpy as jnp
from jax import lax

D = 1024
GROUPS = 3
HPG = 8
DH = 64
BATCH = 4
SPAN_CLOSE = 32
SPREAD_CENTRAL = 4
SPAN_CENTRAL = 32
SPREAD_DISTANT = 16
SPAN_DISTANT = 16
TOKENS = 1024


def level_of(key, dims, split, least, largest):
    def one(position, shards_of):
        heights = jax.random.uniform(jax.random.fold_in(jax.random.fold_in(key, 6), position), (shards_of,), jnp.float32, least / len(split), largest / len(split))
        return jnp.repeat(jnp.exp(heights), dims[position] // shards_of).reshape((-1,) + (1,) * (len(dims) - position - 1))

    factor_of = one(*split[0])
    for cut in split[1:]:
        factor_of = factor_of * one(*cut)
    return factor_of


def centred(key, extent, deviation, bound, cuts=(), kind=jnp.bfloat16):
    drawn = deviation * jax.random.normal(key, extent, jnp.float32)
    if cuts:
        drawn = drawn * level_of(key, extent, cuts, -0.22, 0.18)
    return jnp.clip(drawn, -bound, bound).astype(kind)


def setup_inputs(seed: int = 0) -> dict:
    key_of = jax.random.split(jax.random.key(seed), 9)
    inputs = centred(key_of[0], (BATCH, TOKENS, D), 1.0, 6.0, ((1, 8),))
    norm_gain = jnp.clip(1.0 + 0.18 * jax.random.normal(key_of[1], (D,), jnp.float32), 0.1, 1.9)
    query_weight = centred(key_of[2], (D, GROUPS, HPG, DH), D ** -0.5, 0.1875, ((0, 8), (2, 4)))
    key_weight = centred(key_of[3], (D, GROUPS, HPG, DH), D ** -0.5, 0.1875, ((0, 8), (2, 4)))
    value_weight = centred(key_of[4], (D, GROUPS, HPG, DH), D ** -0.5, 0.1875, ((0, 8), (2, 4)))
    query_gain = jnp.clip(1.0 + 0.18 * jax.random.normal(key_of[5], (GROUPS, DH), jnp.float32), 0.1, 1.9)
    key_gain = jnp.clip(1.0 + 0.18 * jax.random.normal(key_of[6], (GROUPS, DH), jnp.float32), 0.1, 1.9)
    out_weight = centred(key_of[7], (HPG, DH, D), DH ** -0.5, 0.75, ((0, 4), (2, 8)))
    return dict(inputs=inputs, norm_gain=norm_gain, query_weight=query_weight, key_weight=key_weight, value_weight=value_weight, query_gain=query_gain, key_gain=key_gain, out_weight=out_weight)


eps = 1e-06
neg_fill = -1e+30
block_rows = 128

def row_norm(values, gain):
    scaled = values * lax.rsqrt(lax.optimization_barrier(jnp.mean(values * values, axis=-1, keepdims=True)) + eps)
    return scaled * gain

def band_attend(queries, keys, values, dilation, half, slopes):
    seq_len, heads, width = queries.shape
    sub_len = seq_len // dilation

    def to_sub(tensor):
        return tensor.reshape(sub_len, dilation, heads, width).transpose(1, 0, 2, 3)
    query_sub = to_sub(queries)
    key_sub = to_sub(keys)
    value_sub = to_sub(values)
    blocks = -(-sub_len // block_rows)
    padded_len = blocks * block_rows
    key_rows = block_rows + 2 * half
    query_sub = jnp.pad(query_sub, ((0, 0), (0, padded_len - sub_len), (0, 0), (0, 0)))
    key_pad = ((0, 0), (half, padded_len - sub_len + half), (0, 0), (0, 0))
    key_sub = jnp.pad(key_sub, key_pad)
    value_sub = jnp.pad(value_sub, key_pad)
    key_index = jnp.arange(blocks)[:, None] * block_rows + jnp.arange(key_rows)[None, :]
    key_blocks = key_sub[:, key_index]
    value_blocks = value_sub[:, key_index]
    query_blocks = query_sub.reshape(dilation, blocks, block_rows, heads, width)
    scores = jnp.einsum('nbqhe,nbkhe->nbhqk', query_blocks, key_blocks, precision=lax.Precision.HIGHEST) / math.sqrt(width)
    offset = jnp.arange(key_rows)[None, :] - half - jnp.arange(block_rows)[:, None]
    key_place = key_index - half
    allowed = (jnp.abs(offset)[None] <= half) & ((key_place >= 0) & (key_place < sub_len))[:, None, :]
    slant = -slopes[:, None, None] * (jnp.abs(offset).astype(jnp.float32) / float(half))[None]
    scores = jnp.where(allowed[None, :, None], scores + slant[None, None], neg_fill)
    log_total = jax.nn.logsumexp(scores, axis=-1)
    weights = jnp.exp(scores - log_total[..., None])
    result = jnp.einsum('nbhqk,nbkhe->nbqhe', weights, value_blocks, precision=lax.Precision.HIGHEST).reshape(dilation, padded_len, heads, width)[:, :sub_len]
    log_total = log_total.transpose(0, 1, 3, 2).reshape(dilation, padded_len, heads)[:, :sub_len]
    result = result.transpose(1, 0, 2, 3).reshape(seq_len, heads, width)
    log_total = log_total.transpose(1, 0, 2).reshape(seq_len, heads)
    return (result, log_total)

def reference(inputs, norm_gain, query_weight, key_weight, value_weight, query_gain, key_gain, out_weight):
    batch, seq_len, model_width = inputs.shape
    groups = query_weight.shape[1]
    heads = query_weight.shape[2]
    head_width = query_weight.shape[3]
    normed = row_norm(inputs.astype(jnp.float32), norm_gain).astype(jnp.bfloat16)
    normed = normed.reshape(batch * seq_len, model_width)

    def project(weight):
        product = jnp.dot(normed, weight.reshape(model_width, -1), preferred_element_type=jnp.float32)
        return product.astype(jnp.bfloat16).reshape(batch, seq_len, groups, heads, head_width)
    queries = project(query_weight)
    keys = project(key_weight)
    values = project(value_weight)
    slopes = jnp.exp2(-8.0 * jnp.arange(1, heads + 1).astype(jnp.float32) / heads)
    gap_layouts = ((1, SPAN_CLOSE), (SPREAD_CENTRAL, SPAN_CENTRAL), (SPREAD_DISTANT, SPAN_DISTANT))
    results = []
    totals = []
    for group in range(3):
        dilation, half = gap_layouts[group]
        query_group = row_norm(queries[:, :, group].astype(jnp.float32), query_gain[group])
        key_group = row_norm(keys[:, :, group].astype(jnp.float32), key_gain[group])
        value_group = values[:, :, group].astype(jnp.float32)

        def attend_one(trio, dilation=dilation, half=half):
            return band_attend(trio[0], trio[1], trio[2], dilation, half, slopes)
        result, log_total = lax.map(attend_one, (query_group, key_group, value_group))
        results.append(result)
        totals.append(log_total)
    weights = jax.nn.softmax(jnp.stack(totals, 0), axis=0)
    combined = lax.optimization_barrier(jnp.sum(weights[..., None] * jnp.stack(results, 0), axis=0))
    merged = combined.astype(jnp.bfloat16).reshape(batch * seq_len, heads * head_width)
    output = jnp.dot(merged, out_weight.reshape(heads * head_width, model_width), preferred_element_type=jnp.float32)
    return output.astype(jnp.bfloat16).reshape(batch, seq_len, model_width)
```

```python
import functools
import math

import jax
import jax.numpy as jnp
from jax import lax
from jax.experimental import pallas as pl
from jax.experimental.pallas import tpu as pltpu
from jax.sharding import PartitionSpec as P

GAPS = ((1, 32), (4, 32), (16, 16))
EPS = 1e-06
NEG = -1e30
MESH = pl.DeviceIdType.MESH


def halo_plan(length):
    plan = []
    for group, (dilation, half) in enumerate(GAPS):
        reach = dilation * half
        for distance in range(1, -(-reach // length) + 1):
            plan.append((group, distance, min(length, reach - (distance - 1) * length)))
    return sorted(plan, key=lambda item: item[1])


def layer_kernel(
    n, tp, batch, length, heads, width, x_ref, gain_ref, wa_ref, wb_ref, qg_ref, kg_ref, slope_ref, out_ref,
    abuf, bbuf, win0, win1, win2, qn, bias, merged, parts, got,
    rs_send, rs_recv, ring_send, ring_recv, halo_send, halo_recv,
):
    me = lax.axis_index("sp")
    mine = lax.axis_index("tp")
    groups = len(GAPS)
    lanes = heads * width
    rows = batch * length
    half_n = n // 2

    def ring_to_sp(p):
        return jnp.where(p < half_n, 2 * p, 2 * (n - 1 - p) + 1)

    place = jnp.where(me % 2 == 0, me // 2, n - 1 - me // 2)
    forward = ring_to_sp((place + 1) % n)
    backward = ring_to_sp((place + n - 1) % n)
    bufs = (abuf, bbuf)
    firsts = (wa_ref, wb_ref)

    def hop(chunk, way, step):
        owner = ring_to_sp((place + (n - (step - 1) if way == 0 else step - 1)) % n)
        buf = bufs[chunk]
        columns = buf.shape[2]
        cut = pl.ds(0, columns)
        if step == half_n and n % 2 == 0:
            middle = (columns // 2 + 127) // 128 * 128
            cut = pl.ds(0, middle) if way == 0 else pl.ds(middle, columns - middle)
        src = firsts[chunk].at[:, cut] if step == 1 else buf.at[owner, :, cut]
        return pltpu.make_async_remote_copy(
            src_ref=src,
            dst_ref=buf.at[owner, :, cut],
            send_sem=ring_send.at[chunk, way, step - 1],
            recv_sem=ring_recv.at[chunk, way, step - 1],
            device_id={"sp": forward if way == 0 else backward},
            device_id_type=MESH,
        )

    for chunk in range(2):
        for way in range(2):
            hop(chunk, way, 1).start()
    for chunk in range(2):
        bufs[chunk][me] = firsts[chunk][...]

    flat = x_ref[...].reshape(rows, -1).astype(jnp.float32)
    scale = lax.rsqrt(jnp.mean(flat * flat, axis=-1, keepdims=True) + EPS)
    normed = (flat * scale * gain_ref[...]).astype(jnp.bfloat16)

    widths = [length + 2 * d * h for d, h in GAPS]
    starts = [sum(widths[:g]) for g in range(groups)]
    for group, (dilation, half) in enumerate(GAPS):
        reach = dilation * half
        shape = (length, widths[group])
        key = lax.broadcasted_iota(jnp.int32, shape, 1) - reach
        offset = jnp.abs(key - lax.broadcasted_iota(jnp.int32, shape, 0))
        at = key + me * length
        allowed = (offset <= reach) & (at >= 0) & (at < n * length) & ((offset & (dilation - 1)) == 0)
        distance = offset.astype(jnp.float32) / float(reach)
        for head in range(heads):
            value = jnp.where(allowed, -slope_ref[head : head + 1, :1] * distance, NEG)
            bias[head, :, starts[group] : starts[group] + widths[group]] = value

    wins = (win0, win1, win2)
    plan = halo_plan(length)
    for group, distance, count in plan:
        reach = GAPS[group][0] * GAPS[group][1]
        low = reach - (distance - 1) * length - count
        high = reach + distance * length
        blank = jnp.zeros((batch, count, 2 * lanes), jnp.bfloat16)

        @pl.when(me < distance)
        def _(group=group, low=low, count=count, blank=blank):
            wins[group][:, low : low + count, :] = blank

        @pl.when(me + distance >= n)
        def _(group=group, high=high, count=count, blank=blank):
            wins[group][:, high : high + count, :] = blank

    def finish_ring(chunk):
        for way in range(2):
            hop(chunk, way, half_n).wait_recv()

    for step in range(2, half_n + 1):
        for chunk in range(2):
            for way in range(2):
                hop(chunk, way, step - 1).wait_recv()
                hop(chunk, way, step).start()

    row_head = lax.broadcasted_iota(jnp.int32, (lanes, lanes), 0) // width
    column_head = lax.broadcasted_iota(jnp.int32, (lanes, lanes), 1) // width
    same_head = jnp.where(row_head == column_head, 1.0 / width, 0.0)

    def head_norm(block, gain):
        values = block.astype(jnp.bfloat16).astype(jnp.float32)
        mean = jnp.dot(
            values * values, same_head, precision=lax.Precision.HIGHEST, preferred_element_type=jnp.float32
        )
        return values * lax.rsqrt(mean + EPS) * gain

    finish_ring(0)
    depth = abuf.shape[0] * abuf.shape[1]
    key_values = jnp.dot(normed, abuf[...].reshape(depth, -1), preferred_element_type=jnp.float32)
    for group, (dilation, half) in enumerate(GAPS):
        reach = dilation * half
        low = 2 * lanes * group
        keys = head_norm(key_values[:, low : low + lanes], kg_ref[group : group + 1, :])
        values = key_values[:, low + lanes : low + 2 * lanes]
        wins[group][:, reach : reach + length, :lanes] = keys.astype(jnp.bfloat16).reshape(batch, length, lanes)
        wins[group][:, reach : reach + length, lanes:] = values.astype(jnp.bfloat16).reshape(batch, length, lanes)

    def halo(index, up):
        group, distance, count = plan[index]
        reach = GAPS[group][0] * GAPS[group][1]
        win = wins[group]
        if up:
            src = win.at[:, pl.ds(reach + length - count, count), :]
            dst = win.at[:, pl.ds(reach - (distance - 1) * length - count, count), :]
            target = (me + distance) % n
        else:
            src = win.at[:, pl.ds(reach, count), :]
            dst = win.at[:, pl.ds(reach + distance * length, count), :]
            target = (me + n - distance) % n
        side = 0 if up else 1
        return pltpu.make_async_remote_copy(
            src_ref=src,
            dst_ref=dst,
            send_sem=halo_send.at[side, index],
            recv_sem=halo_recv.at[side, index],
            device_id={"sp": target},
            device_id_type=MESH,
        )

    def each_halo(method_up, method_down, inward):
        for index, (group, distance, count) in enumerate(plan):
            above = me + distance < n
            below = me >= distance

            @pl.when(below if inward else above)
            def _(index=index):
                method_up(halo(index, True))

            @pl.when(above if inward else below)
            def _(index=index):
                method_down(halo(index, False))

    each_halo(lambda c: c.start(), lambda c: c.start(), False)

    finish_ring(1)
    factor = 1.0 / math.sqrt(width)
    weights = bbuf[:, :, : groups * lanes].reshape(depth, groups * lanes)
    queries = jnp.dot(normed, weights, preferred_element_type=jnp.float32)
    for group in range(groups):
        block = head_norm(queries[:, lanes * group : lanes * (group + 1)], qg_ref[group : group + 1, :] * factor)
        qn[group] = block.astype(jnp.bfloat16).reshape(batch, length, lanes)

    each_halo(lambda c: c.wait_recv(), lambda c: c.wait_recv(), True)

    lane_head = lax.broadcasted_iota(jnp.int32, (length, lanes), 1) // width

    def attend(b, carry):
        result = jnp.zeros((length, lanes), jnp.float32)
        for head in range(heads):
            here = lane_head == head
            total = jnp.zeros((length, 1), jnp.float32)
            summed = jnp.zeros((length, lanes), jnp.float32)
            for group in range(groups):
                query = qn[group, b]
                query = jnp.where(here, query, jnp.zeros_like(query))
                scores = lax.dot_general(
                    query, wins[group][b, :, :lanes], (((1,), (1,)), ((), ())), preferred_element_type=jnp.float32
                )
                scores = scores + bias[head, :, starts[group] : starts[group] + widths[group]]
                grown = jnp.exp(scores)
                total = total + jnp.sum(grown, axis=-1, keepdims=True)
                summed = summed + jnp.dot(
                    grown.astype(jnp.bfloat16), wins[group][b, :, lanes:], preferred_element_type=jnp.float32
                )
            result = jnp.where(here, summed / total, result)
        merged[b] = result.astype(jnp.bfloat16)
        return carry

    lax.fori_loop(0, batch, attend, 0)

    both = merged[...].reshape(rows, lanes)
    outs = bbuf[:, :, groups * lanes :].reshape(depth, lanes)
    span = depth // tp
    for block in range(tp):
        term = lax.dot_general(
            both, outs[block * span : (block + 1) * span], (((1,), (1,)), ((), ())), preferred_element_type=jnp.float32
        )
        parts[block] = term.astype(jnp.bfloat16)

    def exchange(shift):
        target = (mine + shift) % tp
        return pltpu.make_async_remote_copy(
            src_ref=parts.at[target],
            dst_ref=got.at[shift - 1],
            send_sem=rs_send.at[shift - 1],
            recv_sem=rs_recv.at[shift - 1],
            device_id={"tp": target},
            device_id_type=MESH,
        )

    for shift in range(1, tp):
        exchange(shift).start()
    summed = parts[mine].astype(jnp.float32)
    for shift in range(1, tp):
        exchange(shift).wait_recv()
        summed = summed + got[shift - 1].astype(jnp.float32)
    out_ref[...] = summed.astype(jnp.bfloat16).reshape(batch, length, span)

    for shift in range(1, tp):
        exchange(shift).wait_send()
    for step in range(1, half_n + 1):
        for chunk in range(2):
            for way in range(2):
                hop(chunk, way, step).wait_send()
    each_halo(lambda c: c.wait_send(), lambda c: c.wait_send(), False)


def body(n, tp, inputs, norm_gain, query_weight, key_weight, value_weight, query_gain, key_gain, out_weight):
    batch, length, model = inputs.shape
    share, groups, heads, width = query_weight.shape
    lanes = heads * width
    key_values = jnp.stack(
        [key_weight.reshape(share, groups, lanes), value_weight.reshape(share, groups, lanes)], axis=2
    ).reshape(share, groups * 2 * lanes)
    outs = out_weight.reshape(lanes, -1).T
    rest = jnp.concatenate([query_weight.reshape(share, groups * lanes), outs], axis=1)
    index = lax.axis_index("tp") * heads + jnp.arange(heads)
    slopes = jnp.exp2(-8.0 * (index + 1).astype(jnp.float32) / (heads * tp))
    slopes = jnp.broadcast_to(slopes[:, None], (heads, 128))
    total = sum(length + 2 * d * h for d, h in GAPS)
    windows = [pltpu.VMEM((batch, length + 2 * d * h, 2 * lanes), jnp.bfloat16) for d, h in GAPS]
    plan = halo_plan(length)
    vmem = pl.BlockSpec(memory_space=pltpu.VMEM)
    span = model // tp
    return pl.pallas_call(
        functools.partial(layer_kernel, n, tp, batch, length, heads, width),
        out_shape=jax.ShapeDtypeStruct((batch, length, span), jnp.bfloat16),
        in_specs=[vmem] * 7,
        out_specs=vmem,
        scratch_shapes=[
            pltpu.VMEM((n, share, key_values.shape[1]), jnp.bfloat16),
            pltpu.VMEM((n, share, rest.shape[1]), jnp.bfloat16),
            *windows,
            pltpu.VMEM((groups, batch, length, lanes), jnp.bfloat16),
            pltpu.VMEM((heads, length, total), jnp.float32),
            pltpu.VMEM((batch, length, lanes), jnp.bfloat16),
            pltpu.VMEM((tp, batch * length, span), jnp.bfloat16),
            pltpu.VMEM((tp - 1, batch * length, span), jnp.bfloat16),
            pltpu.SemaphoreType.DMA((tp - 1,)),
            pltpu.SemaphoreType.DMA((tp - 1,)),
            pltpu.SemaphoreType.DMA((2, 2, n // 2)),
            pltpu.SemaphoreType.DMA((2, 2, n // 2)),
            pltpu.SemaphoreType.DMA((2, len(plan))),
            pltpu.SemaphoreType.DMA((2, len(plan))),
        ],
        compiler_params=pltpu.CompilerParams(has_side_effects=True, vmem_limit_bytes=60 * 1024 * 1024),
        name="layer",
    )(
        inputs,
        norm_gain.reshape(1, model),
        key_values,
        rest,
        jnp.tile(query_gain, (1, heads)),
        jnp.tile(key_gain, (1, heads)),
        slopes,
    )


def solution(mesh):
    in_specs = (
        P(None, "sp", None),
        P(),
        P("sp", None, "tp", None),
        P("sp", None, "tp", None),
        P("sp", None, "tp", None),
        P(),
        P(),
        P("tp", None, "sp"),
    )
    out_specs = P(None, "sp", "tp")
    run = functools.partial(body, mesh.shape["sp"], mesh.shape["tp"])
    return jax.shard_map(run, mesh=mesh, in_specs=in_specs, out_specs=out_specs, check_vma=False)
```

```python
import functools
import math

import jax
import jax.numpy as jnp
from jax import lax
from jax.experimental import pallas as pl
from jax.experimental.pallas import tpu as pltpu
from jax.sharding import PartitionSpec as P

GAPS = ((1, 32), (4, 32), (16, 16))
EPS = 1e-06
NEG = -1e30
MESH = pl.DeviceIdType.MESH


def halo_plan(length):
    plan = []
    for group, (dilation, half) in enumerate(GAPS):
        reach = dilation * half
        for distance in range(1, -(-reach // length) + 1):
            plan.append((group, distance, min(length, reach - (distance - 1) * length)))
    return sorted(plan, key=lambda item: item[1])


def layer_kernel(
    n, tp, batch, length, heads, width, x_ref, gain_ref, wa_ref, wb_ref, qg_ref, kg_ref, out_ref,
    abuf, bbuf, win0, win1, win2, qn, bias, sums, totals, parts, got, halves, others,
    near_send, near_recv, rs_send, rs_recv, ring_send, ring_recv, halo_send, halo_recv,
):
    me = lax.axis_index("sp")
    mine = lax.axis_index("tp")
    groups = len(GAPS)
    lanes = heads * width
    rows = batch * length
    half_n = n // 2

    def ring_to_sp(p):
        return jnp.where(p < half_n, 2 * p, 2 * (n - 1 - p) + 1)

    place = jnp.where(me % 2 == 0, me // 2, n - 1 - me // 2)
    forward = ring_to_sp((place + 1) % n)
    backward = ring_to_sp((place + n - 1) % n)
    bufs = (abuf, bbuf)
    firsts = (wa_ref, wb_ref)

    def hop(chunk, way, step):
        owner = ring_to_sp((place + (n - (step - 1) if way == 0 else step - 1)) % n)
        buf = bufs[chunk]
        columns = buf.shape[2]
        cut = pl.ds(0, columns)
        if step == half_n and n % 2 == 0:
            middle = (columns // 2 + 127) // 128 * 128
            cut = pl.ds(0, middle) if way == 0 else pl.ds(middle, columns - middle)
        src = firsts[chunk].at[:, cut] if step == 1 else buf.at[owner, :, cut]
        return pltpu.make_async_remote_copy(
            src_ref=src,
            dst_ref=buf.at[owner, :, cut],
            send_sem=ring_send.at[chunk, way, step - 1],
            recv_sem=ring_recv.at[chunk, way, step - 1],
            device_id={"sp": forward if way == 0 else backward},
            device_id_type=MESH,
        )

    for chunk in range(2):
        for way in range(2):
            hop(chunk, way, 1).start()
    for chunk in range(2):
        bufs[chunk][me] = firsts[chunk][...]

    flat = x_ref[...].reshape(rows, -1).astype(jnp.float32)
    scale = lax.rsqrt(jnp.mean(flat * flat, axis=-1, keepdims=True) + EPS)
    normed = (flat * scale * gain_ref[...]).astype(jnp.bfloat16)

    slopes = []
    for head in range(heads):
        power = -8.0 * (mine * heads + head + 1).astype(jnp.float32) / (heads * tp)
        slopes.append(jnp.exp2(jnp.full((8, 128), power, jnp.float32))[:1, :1])
    widths = [length + 2 * d * h for d, h in GAPS]
    starts = [sum(widths[:g]) for g in range(groups)]
    for group, (dilation, half) in enumerate(GAPS):
        reach = dilation * half
        shape = (length, widths[group])
        key = lax.broadcasted_iota(jnp.int32, shape, 1) - reach
        offset = jnp.abs(key - lax.broadcasted_iota(jnp.int32, shape, 0))
        at = key + me * length
        allowed = (offset <= reach) & (at >= 0) & (at < n * length) & ((offset & (dilation - 1)) == 0)
        distance = offset.astype(jnp.float32) / float(reach)
        for head in range(heads):
            value = jnp.where(allowed, -slopes[head] * distance, NEG)
            bias[head, :, starts[group] : starts[group] + widths[group]] = value

    wins = (win0, win1, win2)
    plan = halo_plan(length)
    for group, distance, count in plan:
        reach = GAPS[group][0] * GAPS[group][1]
        low = reach - (distance - 1) * length - count
        high = reach + distance * length
        blank = jnp.zeros((batch, count, 2 * lanes), jnp.bfloat16)

        @pl.when(me < distance)
        def _(group=group, low=low, count=count, blank=blank):
            wins[group][:, low : low + count, :] = blank

        @pl.when(me + distance >= n)
        def _(group=group, high=high, count=count, blank=blank):
            wins[group][:, high : high + count, :] = blank

    def finish_ring(chunk):
        for way in range(2):
            hop(chunk, way, half_n).wait_recv()

    for step in range(2, half_n + 1):
        for chunk in range(2):
            for way in range(2):
                hop(chunk, way, step - 1).wait_recv()
                hop(chunk, way, step).start()

    row_head = lax.broadcasted_iota(jnp.int32, (lanes, lanes), 0) // width
    column_head = lax.broadcasted_iota(jnp.int32, (lanes, lanes), 1) // width
    same_head = jnp.where(row_head == column_head, 1.0 / width, 0.0)

    def repeated(ref, group):
        return jnp.concatenate([ref[group : group + 1, :]] * heads, axis=1)

    def head_norm(block, gain):
        values = block.astype(jnp.bfloat16).astype(jnp.float32)
        mean = jnp.dot(
            values * values, same_head, precision=lax.Precision.HIGHEST, preferred_element_type=jnp.float32
        )
        return values * lax.rsqrt(mean + EPS) * gain

    finish_ring(0)
    depth = abuf.shape[0] * abuf.shape[1]
    key_values = jnp.dot(normed, abuf[...].reshape(depth, -1), preferred_element_type=jnp.float32)
    for group, (dilation, half) in enumerate(GAPS):
        reach = dilation * half
        low = 2 * lanes * group
        keys = head_norm(key_values[:, low : low + lanes], repeated(kg_ref, group))
        values = key_values[:, low + lanes : low + 2 * lanes]
        wins[group][:, reach : reach + length, :lanes] = keys.astype(jnp.bfloat16).reshape(batch, length, lanes)
        wins[group][:, reach : reach + length, lanes:] = values.astype(jnp.bfloat16).reshape(batch, length, lanes)

    def halo(index, up):
        group, distance, count = plan[index]
        reach = GAPS[group][0] * GAPS[group][1]
        win = wins[group]
        if up:
            src = win.at[:, pl.ds(reach + length - count, count), :]
            dst = win.at[:, pl.ds(reach - (distance - 1) * length - count, count), :]
            target = (me + distance) % n
        else:
            src = win.at[:, pl.ds(reach, count), :]
            dst = win.at[:, pl.ds(reach + distance * length, count), :]
            target = (me + n - distance) % n
        side = 0 if up else 1
        return pltpu.make_async_remote_copy(
            src_ref=src,
            dst_ref=dst,
            send_sem=halo_send.at[side, index],
            recv_sem=halo_recv.at[side, index],
            device_id={"sp": target},
            device_id_type=MESH,
        )

    def each_halo(method_up, method_down, inward, only=None):
        for index, (group, distance, count) in enumerate(plan):
            if only is not None and group != only:
                continue
            above = me + distance < n
            below = me >= distance

            @pl.when(below if inward else above)
            def _(index=index):
                method_up(halo(index, True))

            @pl.when(above if inward else below)
            def _(index=index):
                method_down(halo(index, False))

    each_halo(lambda c: c.start(), lambda c: c.start(), False)

    finish_ring(1)
    factor = 1.0 / math.sqrt(width)
    weights = bbuf[:, :, : groups * lanes].reshape(depth, groups * lanes)
    queries = jnp.dot(normed, weights, preferred_element_type=jnp.float32)
    for group in range(groups):
        block = head_norm(queries[:, lanes * group : lanes * (group + 1)], repeated(qg_ref, group) * factor)
        qn[group] = block.astype(jnp.bfloat16).reshape(batch, length, lanes)

    lane_head = lax.broadcasted_iota(jnp.int32, (length, lanes), 1) // width
    span = depth // tp
    pairs = tp // 2
    parity = mine % 2
    level = mine // 2

    def attend(group, b):
        total = jnp.zeros((length, lanes), jnp.float32)
        summed = jnp.zeros((length, lanes), jnp.float32)
        query_all = qn[group, b]
        for head in range(heads):
            here = lane_head == head
            query = jnp.where(here, query_all, jnp.zeros_like(query_all))
            scores = lax.dot_general(
                query, wins[group][b, :, :lanes], (((1,), (1,)), ((), ())), preferred_element_type=jnp.float32
            )
            grown = jnp.exp(scores + bias[head, :, starts[group] : starts[group] + widths[group]])
            total = jnp.where(here, jnp.sum(grown, axis=-1, keepdims=True), total)
            result = jnp.dot(
                grown.astype(jnp.bfloat16), wins[group][b, :, lanes:], preferred_element_type=jnp.float32
            )
            summed = jnp.where(here, result, summed)
        return summed, total

    def to_partner(b):
        return pltpu.make_async_remote_copy(
            src_ref=parts.at[b, 1 - parity],
            dst_ref=got.at[b],
            send_sem=near_send.at[b],
            recv_sem=near_recv.at[b],
            device_id={"tp": mine + 1 - 2 * parity},
            device_id_type=MESH,
        )

    def to_level(b, shift):
        target = (level + shift) % pairs
        return pltpu.make_async_remote_copy(
            src_ref=halves.at[b, target],
            dst_ref=others.at[b, shift - 1],
            send_sem=rs_send.at[b, shift - 1],
            recv_sem=rs_recv.at[b, shift - 1],
            device_id={"tp": 2 * target + parity},
            device_id_type=MESH,
        )

    def pass_on(b):
        to_partner(b).wait_recv()
        halves[b] = (parts[b, parity].astype(jnp.float32) + got[b].astype(jnp.float32)).astype(jnp.bfloat16)
        for shift in range(1, pairs):
            to_level(b, shift).start()

    outs = bbuf[:, :, groups * lanes :].reshape(depth, lanes)

    def first_groups(group):
        def step(b, carry):
            summed, total = attend(group, b)
            if group == 0:
                sums[b], totals[b] = summed, total
            else:
                sums[b] += summed
                totals[b] += total
            return carry

        return step

    def last_group(b, carry):
        summed, total = attend(groups - 1, b)
        merged = ((sums[b] + summed) / (totals[b] + total)).astype(jnp.bfloat16)
        term = lax.dot_general(merged, outs, (((1,), (1,)), ((), ())), preferred_element_type=jnp.float32)
        for block in range(tp):
            parts[b, block % 2, block // 2] = term[:, block * span : (block + 1) * span].astype(jnp.bfloat16)
        to_partner(b).start()

        @pl.when(b >= 1)
        def _():
            pass_on(b - 1)

        return carry

    for group in range(groups):
        each_halo(lambda c: c.wait_recv(), lambda c: c.wait_recv(), True, group)
        lax.fori_loop(0, batch, last_group if group == groups - 1 else first_groups(group), 0)
    pass_on(batch - 1)

    def finish(b, carry):
        final = parts[b, parity, level].astype(jnp.float32) + got[b, level].astype(jnp.float32)
        for shift in range(1, pairs):
            to_level(b, shift).wait_recv()
            final = final + others[b, shift - 1].astype(jnp.float32)
        out_ref[b] = final.astype(jnp.bfloat16)
        for shift in range(1, pairs):
            to_level(b, shift).wait_send()
        to_partner(b).wait_send()
        return carry

    lax.fori_loop(0, batch, finish, 0)
    for step in range(1, half_n + 1):
        for chunk in range(2):
            for way in range(2):
                hop(chunk, way, step).wait_send()
    each_halo(lambda c: c.wait_send(), lambda c: c.wait_send(), False)


def body(n, tp, inputs, norm_gain, query_weight, key_weight, value_weight, query_gain, key_gain, out_weight):
    batch, length, model = inputs.shape
    share, groups, heads, width = query_weight.shape
    lanes = heads * width
    key_values = jnp.stack(
        [key_weight.reshape(share, groups, lanes), value_weight.reshape(share, groups, lanes)], axis=2
    ).reshape(share, groups * 2 * lanes)
    outs = out_weight.reshape(lanes, -1).T
    rest = jnp.concatenate([query_weight.reshape(share, groups * lanes), outs], axis=1)
    total = sum(length + 2 * d * h for d, h in GAPS)
    windows = [pltpu.VMEM((batch, length + 2 * d * h, 2 * lanes), jnp.bfloat16) for d, h in GAPS]
    plan = halo_plan(length)
    vmem = pl.BlockSpec(memory_space=pltpu.VMEM)
    span = model // tp
    return pl.pallas_call(
        functools.partial(layer_kernel, n, tp, batch, length, heads, width),
        out_shape=jax.ShapeDtypeStruct((batch, length, span), jnp.bfloat16),
        in_specs=[vmem] * 6,
        out_specs=vmem,
        scratch_shapes=[
            pltpu.VMEM((n, share, key_values.shape[1]), jnp.bfloat16),
            pltpu.VMEM((n, share, rest.shape[1]), jnp.bfloat16),
            *windows,
            pltpu.VMEM((groups, batch, length, lanes), jnp.bfloat16),
            pltpu.VMEM((heads, length, total), jnp.float32),
            pltpu.VMEM((batch, length, lanes), jnp.float32),
            pltpu.VMEM((batch, length, lanes), jnp.float32),
            pltpu.VMEM((batch, 2, tp // 2, length, span), jnp.bfloat16),
            pltpu.VMEM((batch, tp // 2, length, span), jnp.bfloat16),
            pltpu.VMEM((batch, tp // 2, length, span), jnp.bfloat16),
            pltpu.VMEM((batch, tp // 2 - 1, length, span), jnp.bfloat16),
            pltpu.SemaphoreType.DMA((batch,)),
            pltpu.SemaphoreType.DMA((batch,)),
            pltpu.SemaphoreType.DMA((batch, tp // 2 - 1)),
            pltpu.SemaphoreType.DMA((batch, tp // 2 - 1)),
            pltpu.SemaphoreType.DMA((2, 2, n // 2)),
            pltpu.SemaphoreType.DMA((2, 2, n // 2)),
            pltpu.SemaphoreType.DMA((2, len(plan))),
            pltpu.SemaphoreType.DMA((2, len(plan))),
        ],
        compiler_params=pltpu.CompilerParams(has_side_effects=True, vmem_limit_bytes=60 * 1024 * 1024),
        name="layer",
    )(
        inputs,
        norm_gain.reshape(1, model),
        key_values,
        rest,
        query_gain,
        key_gain,
    )


def solution(mesh):
    in_specs = (
        P(None, "sp", None),
        P(),
        P("sp", None, "tp", None),
        P("sp", None, "tp", None),
        P("sp", None, "tp", None),
        P(),
        P(),
        P("tp", None, "sp"),
    )
    out_specs = P(None, "sp", "tp")
    run = functools.partial(body, mesh.shape["sp"], mesh.shape["tp"])
    return jax.shard_map(run, mesh=mesh, in_specs=in_specs, out_specs=out_specs, check_vma=False)
```

```python
import functools
import math

import jax
import jax.numpy as jnp
from jax import lax
from jax.experimental import pallas as pl
from jax.experimental.pallas import tpu as pltpu
from jax.sharding import PartitionSpec as P

GAPS = ((1, 32), (4, 32), (16, 16))
EPS = 1e-06
NEG = -1e30
MESH = pl.DeviceIdType.MESH


def halo_plan(length):
    plan = []
    for group, (dilation, half) in enumerate(GAPS):
        reach = dilation * half
        for distance in range(1, -(-reach // length) + 1):
            plan.append((group, distance, min(length, reach - (distance - 1) * length)))
    return sorted(plan, key=lambda item: item[1])


def layer_kernel(
    n, tp, batch, length, heads, width, x_ref, gain_ref, wa_ref, wb_ref, qg_ref, kg_ref, out_ref,
    abuf, bbuf, win0, win1, win2, qn, bias, sums, totals, parts, got, halves, others,
    near_send, near_recv, rs_send, rs_recv, ring_send, ring_recv, halo_send, halo_recv,
):
    me = lax.axis_index("sp")
    mine = lax.axis_index("tp")
    groups = len(GAPS)
    lanes = heads * width
    rows = batch * length
    half_n = n // 2

    def ring_to_sp(p):
        return jnp.where(p < half_n, 2 * p, 2 * (n - 1 - p) + 1)

    place = jnp.where(me % 2 == 0, me // 2, n - 1 - me // 2)
    forward = ring_to_sp((place + 1) % n)
    backward = ring_to_sp((place + n - 1) % n)
    bufs = (abuf, bbuf)
    firsts = (wa_ref, wb_ref)

    def hop(chunk, way, step):
        owner = ring_to_sp((place + (n - (step - 1) if way == 0 else step - 1)) % n)
        buf = bufs[chunk]
        columns = buf.shape[2]
        cut = pl.ds(0, columns)
        if step == half_n and n % 2 == 0:
            middle = (columns // 2 + 127) // 128 * 128
            cut = pl.ds(0, middle) if way == 0 else pl.ds(middle, columns - middle)
        src = firsts[chunk].at[:, cut] if step == 1 else buf.at[owner, :, cut]
        return pltpu.make_async_remote_copy(
            src_ref=src,
            dst_ref=buf.at[owner, :, cut],
            send_sem=ring_send.at[chunk, way, step - 1],
            recv_sem=ring_recv.at[chunk, way, step - 1],
            device_id={"sp": forward if way == 0 else backward},
            device_id_type=MESH,
        )

    barrier = pltpu.get_barrier_semaphore()

    def greet(target):
        pl.semaphore_signal(barrier, inc=1, device_id=target, device_id_type=MESH)

    greet({"sp": forward})
    greet({"sp": backward})
    greet({"tp": mine + 1 - 2 * (mine % 2)})
    for shift in range(1, tp // 2):
        greet({"tp": (mine + 2 * shift) % tp})
    plan = halo_plan(length)
    for distance in sorted({item[1] for item in plan}):

        @pl.when(me + distance < n)
        def _(distance=distance):
            greet({"sp": me + distance})

        @pl.when(me >= distance)
        def _(distance=distance):
            greet({"sp": me - distance})

    count = 2 + tp // 2
    for distance in sorted({item[1] for item in plan}):
        count = count + jnp.where(me + distance < n, 1, 0) + jnp.where(me >= distance, 1, 0)
    pl.semaphore_wait(barrier, count)

    for chunk in range(2):
        for way in range(2):
            hop(chunk, way, 1).start()
    for chunk in range(2):
        bufs[chunk][me] = firsts[chunk][...]

    flat = x_ref[...].reshape(rows, -1).astype(jnp.float32)
    scale = lax.rsqrt(jnp.mean(flat * flat, axis=-1, keepdims=True) + EPS)
    normed = (flat * scale * gain_ref[...]).astype(jnp.bfloat16)

    slopes = []
    for head in range(heads):
        power = -8.0 * (mine * heads + head + 1).astype(jnp.float32) / (heads * tp)
        slopes.append(jnp.exp2(jnp.full((8, 128), power, jnp.float32))[:1, :1])
    widths = [length + 2 * d * h for d, h in GAPS]
    starts = [sum(widths[:g]) for g in range(groups)]
    for group, (dilation, half) in enumerate(GAPS):
        reach = dilation * half
        shape = (length, widths[group])
        key = lax.broadcasted_iota(jnp.int32, shape, 1) - reach
        offset = jnp.abs(key - lax.broadcasted_iota(jnp.int32, shape, 0))
        at = key + me * length
        allowed = (offset <= reach) & (at >= 0) & (at < n * length) & ((offset & (dilation - 1)) == 0)
        distance = offset.astype(jnp.float32) / float(reach)
        for head in range(heads):
            value = jnp.where(allowed, -slopes[head] * distance, NEG)
            bias[head, :, starts[group] : starts[group] + widths[group]] = value

    wins = (win0, win1, win2)
    for group, distance, count in plan:
        reach = GAPS[group][0] * GAPS[group][1]
        low = reach - (distance - 1) * length - count
        high = reach + distance * length
        blank = jnp.zeros((batch, count, 2 * lanes), jnp.bfloat16)

        @pl.when(me < distance)
        def _(group=group, low=low, count=count, blank=blank):
            wins[group][:, low : low + count, :] = blank

        @pl.when(me + distance >= n)
        def _(group=group, high=high, count=count, blank=blank):
            wins[group][:, high : high + count, :] = blank

    def finish_ring(chunk):
        for way in range(2):
            hop(chunk, way, half_n).wait_recv()

    def advance(chunk, step):
        if 2 <= step <= half_n:
            for way in range(2):
                hop(chunk, way, step - 1).wait_recv()
                hop(chunk, way, step).start()

    for step in range(2, half_n + 1):
        advance(0, step)
        advance(1, step - 1)

    row_head = lax.broadcasted_iota(jnp.int32, (lanes, lanes), 0) // width
    column_head = lax.broadcasted_iota(jnp.int32, (lanes, lanes), 1) // width
    same_head = jnp.where(row_head == column_head, 1.0 / width, 0.0)

    def repeated(ref, group):
        return jnp.concatenate([ref[group : group + 1, :]] * heads, axis=1)

    def head_norm(block, gain):
        values = block.astype(jnp.bfloat16).astype(jnp.float32)
        mean = jnp.dot(
            values * values, same_head, precision=lax.Precision.HIGHEST, preferred_element_type=jnp.float32
        )
        return values * lax.rsqrt(mean + EPS) * gain

    finish_ring(0)
    depth = abuf.shape[0] * abuf.shape[1]
    def halo(index, up):
        group, distance, count = plan[index]
        reach = GAPS[group][0] * GAPS[group][1]
        win = wins[group]
        if up:
            src = win.at[:, pl.ds(reach + length - count, count), :]
            dst = win.at[:, pl.ds(reach - (distance - 1) * length - count, count), :]
            target = (me + distance) % n
        else:
            src = win.at[:, pl.ds(reach, count), :]
            dst = win.at[:, pl.ds(reach + distance * length, count), :]
            target = (me + n - distance) % n
        side = 0 if up else 1
        return pltpu.make_async_remote_copy(
            src_ref=src,
            dst_ref=dst,
            send_sem=halo_send.at[side, index],
            recv_sem=halo_recv.at[side, index],
            device_id={"sp": target},
            device_id_type=MESH,
        )

    def each_halo(method_up, method_down, inward, only=None):
        for index, (group, distance, count) in enumerate(plan):
            if only is not None and group != only:
                continue
            above = me + distance < n
            below = me >= distance

            @pl.when(below if inward else above)
            def _(index=index):
                method_up(halo(index, True))

            @pl.when(above if inward else below)
            def _(index=index):
                method_down(halo(index, False))

    for group in reversed(range(groups)):
        reach = GAPS[group][0] * GAPS[group][1]
        low = 2 * lanes * group
        weights = abuf[:, :, low : low + 2 * lanes].reshape(depth, 2 * lanes)
        key_values = jnp.dot(normed, weights, preferred_element_type=jnp.float32)
        keys = head_norm(key_values[:, :lanes], repeated(kg_ref, group))
        values = key_values[:, lanes:]
        wins[group][:, reach : reach + length, :lanes] = keys.astype(jnp.bfloat16).reshape(batch, length, lanes)
        wins[group][:, reach : reach + length, lanes:] = values.astype(jnp.bfloat16).reshape(batch, length, lanes)
        if group == groups - 1:
            advance(1, half_n)
        each_halo(lambda c: c.start(), lambda c: c.start(), False, group)

    finish_ring(1)
    factor = 1.0 / math.sqrt(width)
    weights = bbuf[:, :, : groups * lanes].reshape(depth, groups * lanes)
    queries = jnp.dot(normed, weights, preferred_element_type=jnp.float32)
    for group in range(groups):
        block = head_norm(queries[:, lanes * group : lanes * (group + 1)], repeated(qg_ref, group) * factor)
        qn[group] = block.astype(jnp.bfloat16).reshape(batch, length, lanes)

    lane_head = lax.broadcasted_iota(jnp.int32, (length, lanes), 1) // width
    span = depth // tp
    pairs = tp // 2
    parity = mine % 2
    level = mine // 2

    def attend(group, b):
        total = jnp.zeros((length, lanes), jnp.float32)
        summed = jnp.zeros((length, lanes), jnp.float32)
        query_all = qn[group, b]
        for head in range(heads):
            here = lane_head == head
            query = jnp.where(here, query_all, jnp.zeros_like(query_all))
            scores = lax.dot_general(
                query, wins[group][b, :, :lanes], (((1,), (1,)), ((), ())), preferred_element_type=jnp.float32
            )
            grown = jnp.exp(scores + bias[head, :, starts[group] : starts[group] + widths[group]])
            total = jnp.where(here, jnp.sum(grown, axis=-1, keepdims=True), total)
            result = jnp.dot(
                grown.astype(jnp.bfloat16), wins[group][b, :, lanes:], preferred_element_type=jnp.float32
            )
            summed = jnp.where(here, result, summed)
        return summed, total

    def to_partner(b):
        return pltpu.make_async_remote_copy(
            src_ref=parts.at[b, 1 - parity],
            dst_ref=got.at[b],
            send_sem=near_send.at[b],
            recv_sem=near_recv.at[b],
            device_id={"tp": mine + 1 - 2 * parity},
            device_id_type=MESH,
        )

    def to_level(b, shift):
        target = (level + shift) % pairs
        return pltpu.make_async_remote_copy(
            src_ref=halves.at[b, target],
            dst_ref=others.at[b, shift - 1],
            send_sem=rs_send.at[b, shift - 1],
            recv_sem=rs_recv.at[b, shift - 1],
            device_id={"tp": 2 * target + parity},
            device_id_type=MESH,
        )

    def pass_on(b):
        to_partner(b).wait_recv()
        halves[b] = (parts[b, parity].astype(jnp.float32) + got[b].astype(jnp.float32)).astype(jnp.bfloat16)
        for shift in range(1, pairs):
            to_level(b, shift).start()

    outs = bbuf[:, :, groups * lanes :].reshape(depth, lanes)

    def first_groups(group):
        def step(b, carry):
            summed, total = attend(group, b)
            if group == groups - 1:
                sums[b], totals[b] = summed, total
            else:
                sums[b] += summed
                totals[b] += total
            return carry

        return step

    def last_group(b, carry):
        summed, total = attend(0, b)
        merged = ((sums[b] + summed) / (totals[b] + total)).astype(jnp.bfloat16)
        term = lax.dot_general(merged, outs, (((1,), (1,)), ((), ())), preferred_element_type=jnp.float32)
        for block in range(tp):
            parts[b, block % 2, block // 2] = term[:, block * span : (block + 1) * span].astype(jnp.bfloat16)
        to_partner(b).start()

        @pl.when(b >= 1)
        def _():
            pass_on(b - 1)

        return carry

    for group in reversed(range(groups)):
        each_halo(lambda c: c.wait_recv(), lambda c: c.wait_recv(), True, group)
        lax.fori_loop(0, batch, last_group if group == 0 else first_groups(group), 0)
    pass_on(batch - 1)

    def finish(b, carry):
        final = parts[b, parity, level].astype(jnp.float32) + got[b, level].astype(jnp.float32)
        for shift in range(1, pairs):
            to_level(b, shift).wait_recv()
            final = final + others[b, shift - 1].astype(jnp.float32)
        out_ref[b] = final.astype(jnp.bfloat16)
        for shift in range(1, pairs):
            to_level(b, shift).wait_send()
        to_partner(b).wait_send()
        return carry

    lax.fori_loop(0, batch, finish, 0)
    for step in range(1, half_n + 1):
        for chunk in range(2):
            for way in range(2):
                hop(chunk, way, step).wait_send()
    each_halo(lambda c: c.wait_send(), lambda c: c.wait_send(), False)


def body(n, tp, inputs, norm_gain, query_weight, key_weight, value_weight, query_gain, key_gain, out_weight):
    batch, length, model = inputs.shape
    share, groups, heads, width = query_weight.shape
    lanes = heads * width
    key_values = jnp.stack(
        [key_weight.reshape(share, groups, lanes), value_weight.reshape(share, groups, lanes)], axis=2
    ).reshape(share, groups * 2 * lanes)
    outs = out_weight.reshape(lanes, -1).T
    rest = jnp.concatenate([query_weight.reshape(share, groups * lanes), outs], axis=1)
    total = sum(length + 2 * d * h for d, h in GAPS)
    windows = [pltpu.VMEM((batch, length + 2 * d * h, 2 * lanes), jnp.bfloat16) for d, h in GAPS]
    plan = halo_plan(length)
    vmem = pl.BlockSpec(memory_space=pltpu.VMEM)
    span = model // tp
    return pl.pallas_call(
        functools.partial(layer_kernel, n, tp, batch, length, heads, width),
        out_shape=jax.ShapeDtypeStruct((batch, length, span), jnp.bfloat16),
        in_specs=[vmem] * 6,
        out_specs=vmem,
        scratch_shapes=[
            pltpu.VMEM((n, share, key_values.shape[1]), jnp.bfloat16),
            pltpu.VMEM((n, share, rest.shape[1]), jnp.bfloat16),
            *windows,
            pltpu.VMEM((groups, batch, length, lanes), jnp.bfloat16),
            pltpu.VMEM((heads, length, total), jnp.float32),
            pltpu.VMEM((batch, length, lanes), jnp.float32),
            pltpu.VMEM((batch, length, lanes), jnp.float32),
            pltpu.VMEM((batch, 2, tp // 2, length, span), jnp.bfloat16),
            pltpu.VMEM((batch, tp // 2, length, span), jnp.bfloat16),
            pltpu.VMEM((batch, tp // 2, length, span), jnp.bfloat16),
            pltpu.VMEM((batch, tp // 2 - 1, length, span), jnp.bfloat16),
            pltpu.SemaphoreType.DMA((batch,)),
            pltpu.SemaphoreType.DMA((batch,)),
            pltpu.SemaphoreType.DMA((batch, tp // 2 - 1)),
            pltpu.SemaphoreType.DMA((batch, tp // 2 - 1)),
            pltpu.SemaphoreType.DMA((2, 2, n // 2)),
            pltpu.SemaphoreType.DMA((2, 2, n // 2)),
            pltpu.SemaphoreType.DMA((2, len(plan))),
            pltpu.SemaphoreType.DMA((2, len(plan))),
        ],
        compiler_params=pltpu.CompilerParams(collective_id=0, has_side_effects=True, vmem_limit_bytes=60 * 1024 * 1024),
        name="layer",
    )(
        inputs,
        norm_gain.reshape(1, model),
        key_values,
        rest,
        query_gain,
        key_gain,
    )


def solution(mesh):
    in_specs = (
        P(None, "sp", None),
        P(),
        P("sp", None, "tp", None),
        P("sp", None, "tp", None),
        P("sp", None, "tp", None),
        P(),
        P(),
        P("tp", None, "sp"),
    )
    out_specs = P(None, "sp", "tp")
    run = functools.partial(body, mesh.shape["sp"], mesh.shape["tp"])
    return jax.shard_map(run, mesh=mesh, in_specs=in_specs, out_specs=out_specs, check_vma=False)
```
